32 devices in a mesh: ep: 8 (over z, y), tp: 4 (over x, core).
Axes of the slice: x: 2, y: 2, z: 4, core: 2. Of those that a mesh axis runs over, the one named last changes fastest.
Arguments:
- mixer_input: bfloat16 [4096, 2048], P('ep'), may hold values from -6 to 6
- mixer_gain: bfloat16 [2048], replicated, may hold values from 0.099609375 to 1.8984375
- pool_in: bfloat16 [2048, 1024], P(None, 'tp'), may hold values from -0.125 to 0.125
- pool_map: bfloat16 [4, 256, 256], P('tp'), may hold values from -0.375 to 0.375
- pool_scale: bfloat16 [1024], P('tp'), may hold values from 0.099609375 to 1.8984375
- pool_out: bfloat16 [1024, 2048], P('tp'), may hold values from -0.1875 to 0.1875
- expert_input: bfloat16 [3072, 2048], P('ep'), may hold values from -6 to 6
- expert_gain: bfloat16 [2048], replicated, may hold values from 0.099609375 to 1.8984375
- group_router: bfloat16 [2048, 4], replicated, may hold values from -0.125 to 0.125
- expert_router: bfloat16 [2048, 8], replicated, may hold values from -0.125 to 0.125
- routes: int32 [3072, 2], P('ep'), may hold values from 0 to 7, all different within a row; in each aligned block of 96 rows (0 to 95, 96 to 191, ...) at most 48 rows name the same one
- gate_weight: bfloat16 [8, 2048, 1024], P('ep', None, 'tp'), may hold values from -0.125 to 0.125
- up_weight: bfloat16 [8, 2048, 1024], P('ep', None, 'tp'), may hold values from -0.125 to 0.125
- down_weight: bfloat16 [8, 1024, 2048], P('ep', 'tp'), may hold values from -0.1875 to 0.1875
Outputs:
- mixer_output: bfloat16 [4096, 2048], P(('ep', 'tp'))
- expert_output: bfloat16 [3072, 2048], P(('ep', 'tp'))
The draws below stay inside these ranges and needn't reach their ends.
Inputs may be any that keep to these rules, and one draw needn't show every extreme that they name: `routes`: each row names two different experts. In each aligned block of 96 rows no expert is named more than 48 times, a bound that some block reaches.
All inputs are finite; a program needn't handle non-finite values.
Results may differ from the reference program's by a relative error of at most 0.01.
Values may be sent and summed in bfloat16 or wider, within the bound.
A program may use at most 64 MiB of HBM per device.

```python
import math
import jax
import jax.numpy as jnp
import numpy as np
from jax import lax

D = 2048
MIX_A = 1024
POOL_GROUPS = 4
POOL_CH = 256
RIM = 15
HID = 1024
EXPERT_GROUPS = 4
EXPERTS = 8
TOK_A = 4096
TB_DEV = 96
TOK_B = 3072
CAPQ = 48
N_TP = 4


def levels(stream_key, extent, shards, least, largest):
    loudness, own = 1.0, jax.random.fold_in(stream_key, 6)
    for dim, parts in shards:
        draws = jnp.exp(jax.random.uniform(jax.random.fold_in(own, dim), (parts,), jnp.float32, least / len(shards), largest / len(shards)))
        loudness = loudness * jnp.repeat(draws, extent[dim] // parts).reshape([-1 if axis == dim else 1 for axis in range(len(extent))])
    return loudness


def shared_out(own_key, own, number, rows, number_of, top, bound, lean):
    order = jax.random.permutation(own_key, number_of)
    crowded, usual = portions_of(number_of, rows * top, bound, lean, True), portions_of(number_of, rows * top, bound, lean, False)
    places = jnp.arange(number_of)

    def named(lengths, turn):
        used = int((lengths > 0).sum())
        fixed = max(1, used // 4)
        shifted = fixed + (places - fixed + turn * (used - fixed)) % max(1, number_of - fixed)
        return jnp.zeros((number_of,), jnp.int32).at[order[jnp.where(places < fixed, places, shifted)]].set(jnp.asarray(lengths, jnp.int32))

    lengths = jnp.where(number % 4 == 0, named(crowded, number // 4), named(usual, number - number // 4 - 1))
    mixed = jax.random.permutation(jax.random.fold_in(own, 3), number_of)
    giver, sink = mixed[0:number_of // 2 * 2:2], mixed[1:number_of // 2 * 2:2]
    room = jnp.minimum(lengths[giver] - 1, bound - lengths[sink]) // 2
    room = jnp.where((giver == order[0]) | (sink == order[0]) | (lengths[sink] == 0), 0, jnp.maximum(room, 0))
    shifted = jax.random.randint(jax.random.fold_in(own, 4), (number_of // 2,), 0, 1 << 20) % (room + 1)
    lengths = lengths.at[giver].add(-shifted).at[sink].add(shifted)
    labels = jnp.searchsorted(jnp.cumsum(lengths), jnp.arange(rows * top), side="right").astype(jnp.int32)
    grid = labels.reshape(top, rows).T
    grid = grid[jax.random.permutation(jax.random.fold_in(own, 1), rows)]
    turn = jax.random.randint(jax.random.fold_in(own, 2), (rows, 1), 0, top)
    return jnp.take_along_axis(grid, (jnp.arange(top)[None, :] + turn) % top, axis=1)


def portions_of(number_of, total, most, lean, full):
    loads = [(1 << 20) // math.isqrt(grade ** lean) + 1 for grade in range(1, number_of + 1)]
    largest = most if full else min(most, max(-(-total // number_of), total * loads[0] // sum(loads)))
    least = 1 if total - largest >= number_of - 1 else 0
    holding, spare = [largest] + [least] * (number_of - 1), total - largest - least * (number_of - 1)
    while spare > 0:
        movable = [i for i in range(1, number_of) if holding[i] < largest] or [i for i in range(1, number_of) if holding[i] < most]
        mass, budget = sum([loads[i] for i in movable]), spare
        for i in movable:
            more = min(most - holding[i], max(1, budget * loads[i] // mass), spare)
            holding[i] = holding[i] + more
            spare = spare - more
    return np.array(holding)


def normal_values(key, extent, spread, most, shards=(), held_as=jnp.bfloat16):
    entries = spread * jax.random.normal(key, extent, jnp.float32)
    if shards:
        entries = entries * levels(key, extent, shards, -0.22, 0.18)
    return jnp.clip(entries, -most, most).astype(held_as)


def setup_inputs(seed: int = 0) -> dict:
    key_of = jax.random.split(jax.random.key(seed), 15)
    mixer_input = normal_values(key_of[0], (TOK_A, D), 1.0, 6.0, ((0, 8),))
    mixer_gain = jnp.clip(1.0 + 0.18 * jax.random.normal(key_of[1], (D,), jnp.float32), 0.099609375, 1.8984375).astype(jnp.bfloat16)
    pool_in = normal_values(key_of[2], (D, MIX_A), D ** -0.5, 0.125, ((1, 4),))
    pool_map = normal_values(key_of[3], (POOL_GROUPS, POOL_CH, POOL_CH), POOL_CH ** -0.5, 0.375, ((0, 4),))
    pool_scale = jnp.clip(1.0 + 0.18 * jax.random.normal(key_of[4], (MIX_A,), jnp.float32), 0.099609375, 1.8984375).astype(jnp.bfloat16)
    pool_out = normal_values(key_of[5], (MIX_A, D), MIX_A ** -0.5, 0.1875, ((0, 4),))
    expert_input = normal_values(key_of[6], (TOK_B, D), 1.0, 6.0, ((0, 8),))
    expert_gain = jnp.clip(1.0 + 0.18 * jax.random.normal(key_of[7], (D,), jnp.float32), 0.099609375, 1.8984375).astype(jnp.bfloat16)
    group_router = normal_values(key_of[8], (D, EXPERT_GROUPS), D ** -0.5, 0.125)
    expert_router = normal_values(key_of[9], (D, EXPERTS), D ** -0.5, 0.125)
    routes_keys = jax.random.split(jax.random.fold_in(key_of[10], 1), TOK_B // TB_DEV)
    routes_turns = jax.random.permutation(jax.random.fold_in(key_of[10], 3), TOK_B // TB_DEV)
    routes = jax.vmap(lambda own, number: shared_out(jax.random.fold_in(key_of[10], 2), own, number, TB_DEV, EXPERTS, 2, CAPQ, 2))(routes_keys, routes_turns).reshape((TOK_B, 2))
    gate_weight = normal_values(key_of[11], (EXPERTS, D, HID), D ** -0.5, 0.125, ((0, 8), (2, 4)))
    up_weight = normal_values(key_of[12], (EXPERTS, D, HID), D ** -0.5, 0.125, ((0, 8), (2, 4)))
    down_weight = normal_values(key_of[13], (EXPERTS, HID, D), HID ** -0.5, 0.1875, ((0, 8), (1, 4)))
    return {"mixer_input": mixer_input, "mixer_gain": mixer_gain, "pool_in": pool_in, "pool_map": pool_map, "pool_scale": pool_scale, "pool_out": pool_out, "expert_input": expert_input, "expert_gain": expert_gain, "group_router": group_router, "expert_router": expert_router, "routes": routes, "gate_weight": gate_weight, "up_weight": up_weight, "down_weight": down_weight}


EPS = 1e-06
block_rows = 128

def norm_rows(values, gain):
    floats = values.astype(jnp.float32)
    scale = lax.rsqrt(lax.optimization_barrier(jnp.mean(floats * floats, axis=-1, keepdims=True)) + EPS)
    return (floats * scale * gain.astype(jnp.float32)).astype(jnp.bfloat16)

def route_weights(rows, group_router, expert_router, route_rows):
    group_logits = jnp.dot(rows, group_router, preferred_element_type=jnp.float32)
    expert_logits = jnp.dot(rows, expert_router, preferred_element_type=jnp.float32)
    groups = group_logits.shape[1]
    experts = expert_logits.shape[1]
    member = (jnp.arange(experts, dtype=jnp.int32)[:, None] // (experts // groups) == jnp.arange(groups, dtype=jnp.int32)[None, :]).astype(jnp.float32)
    group_exp = jnp.exp(group_logits)
    group_prob = group_exp / lax.optimization_barrier(jnp.sum(group_exp, axis=1, keepdims=True))
    expert_exp = jnp.exp(expert_logits)
    within = jnp.dot(expert_exp, member, precision=lax.Precision.HIGHEST)
    prob = expert_exp * jnp.dot(group_prob / within, member.T, precision=lax.Precision.HIGHEST)
    chosen = (route_rows[:, :, None] == jnp.arange(experts, dtype=jnp.int32)[None, None, :]).astype(jnp.float32)
    picked = lax.optimization_barrier(jnp.sum(chosen * prob[:, None, :], axis=2))
    return picked / lax.optimization_barrier(jnp.sum(picked, axis=1, keepdims=True))

def reference(mixer_input, mixer_gain, pool_in, pool_map, pool_scale, pool_out, expert_input, expert_gain, group_router, expert_router, routes, gate_weight, up_weight, down_weight):
    normed = norm_rows(mixer_input, mixer_gain)
    pooled_in = jnp.dot(normed, pool_in, preferred_element_type=jnp.float32).astype(jnp.bfloat16)
    tokens = pooled_in.shape[0]
    floats = pooled_in.astype(jnp.float32).reshape(tokens, POOL_GROUPS, POOL_CH)
    padded = jnp.concatenate([jnp.zeros((RIM, POOL_GROUPS, POOL_CH), jnp.float32), floats], axis=0)
    position = jnp.arange(tokens, dtype=jnp.int32)
    group_list = []
    for group in range(POOL_GROUPS):
        window = 2 ** (group + 1)
        window_sum = jnp.zeros((tokens, POOL_CH), jnp.float32)
        for offset in range(window):
            window_sum = window_sum + padded[RIM - offset:RIM - offset + tokens, group]
        counts = jnp.minimum(position + 1, window).astype(jnp.float32)
        group_list.append(window_sum / counts[:, None] - floats[:, group])
    pooled = jnp.stack(group_list, axis=1).astype(jnp.bfloat16)
    mapped = jnp.einsum('tgc,gce->tge', pooled.astype(jnp.float32), pool_map.astype(jnp.float32))
    mixed = (mapped.reshape(tokens, MIX_A) * pool_scale.astype(jnp.float32)).astype(jnp.bfloat16)
    quarter = MIX_A // N_TP
    mixer_sum = jnp.zeros((tokens, D), jnp.float32)
    for part in range(N_TP):
        partial_value = jnp.dot(mixed[:, part * quarter:(part + 1) * quarter], pool_out[part * quarter:(part + 1) * quarter], preferred_element_type=jnp.float32).astype(jnp.bfloat16)
        partial_value = lax.optimization_barrier(partial_value)
        mixer_sum = mixer_sum + partial_value.astype(jnp.float32)
    mixer_output = mixer_sum.astype(jnp.bfloat16)
    normed_exp = norm_rows(expert_input, expert_gain)
    weights = route_weights(normed_exp, group_router, expert_router, routes)
    tokens_b = normed_exp.shape[0]
    flat = routes.reshape(-1).astype(jnp.int32)
    assigned = flat.shape[0]
    owner = (jnp.arange(assigned, dtype=jnp.int32) // 2).astype(jnp.int32)
    order = jnp.argsort(flat, stable=True).astype(jnp.int32)
    sorted_expert = flat[order]
    sorted_owner = owner[order]
    counts_all = lax.optimization_barrier(jnp.sum((flat[:, None] == jnp.arange(EXPERTS, dtype=jnp.int32)[None, :]).astype(jnp.int32), axis=0))
    starts = (jnp.cumsum(counts_all) - counts_all).astype(jnp.int32)
    padded_counts = (counts_all + block_rows - 1) // block_rows * block_rows
    pad_starts = (jnp.cumsum(padded_counts) - padded_counts).astype(jnp.int32)
    pad_ends = pad_starts + padded_counts
    dest = (pad_starts[sorted_expert] + jnp.arange(assigned, dtype=jnp.int32) - starts[sorted_expert]).astype(jnp.int32)
    blocks = (assigned + EXPERTS * (block_rows - 1) + block_rows - 1) // block_rows
    buffer = jnp.zeros((blocks * block_rows, D), jnp.bfloat16).at[dest].set(normed_exp[sorted_owner])
    block_start = jnp.arange(blocks, dtype=jnp.int32) * block_rows
    block_expert = jnp.clip(lax.optimization_barrier(jnp.sum((pad_ends[None, :] <= block_start[:, None]).astype(jnp.int32), axis=1)), 0, EXPERTS - 1).astype(jnp.int32)
    hid_part = HID // N_TP

    def expert_block(pair):
        rows_here, expert = pair
        gate = jnp.dot(rows_here, gate_weight[expert], preferred_element_type=jnp.float32)
        upward = jnp.dot(rows_here, up_weight[expert], preferred_element_type=jnp.float32)
        hidden = (jax.nn.silu(gate) * upward).astype(jnp.bfloat16)
        result = jnp.zeros((block_rows, D), jnp.float32)
        for part in range(N_TP):
            partial_value = jnp.dot(hidden[:, part * hid_part:(part + 1) * hid_part], down_weight[expert, part * hid_part:(part + 1) * hid_part], preferred_element_type=jnp.float32).astype(jnp.bfloat16)
            partial_value = lax.optimization_barrier(partial_value)
            result = result + partial_value.astype(jnp.float32)
        return result.astype(jnp.bfloat16)
    results = lax.map(expert_block, (buffer.reshape(blocks, block_rows, D), block_expert)).reshape(-1, D)
    per_copy = results[dest].astype(jnp.float32)
    copy_weight = weights.reshape(-1)[order]
    expert_sum = jnp.zeros((tokens_b, D), jnp.float32).at[sorted_owner].add(per_copy * copy_weight[:, None])
    return (mixer_output, expert_sum.astype(jnp.bfloat16))
```

```python
import jax
import jax.numpy as jnp
from jax import lax
from jax.sharding import PartitionSpec as P

RIM = 15
EPS = 1e-06


def passed_along(value, axis, steps):
    count = lax.axis_size(axis)
    leading, last = (max(0, -steps), min(count, count - steps))
    return lax.ppermute(value, axis, [(source, source + steps) for source in range(leading, last)])


def swapped(value, axis, mask):
    count = lax.axis_size(axis)
    return lax.ppermute(value, axis, [(source, source ^ mask) for source in range(count)])


def masks_of(axis):
    count, masks = lax.axis_size(axis), []
    while count > 1:
        count //= 2
        masks.append(count)
    return masks


def norm_rows(values, gain):
    floats = values.astype(jnp.float32)
    scale = lax.rsqrt(jnp.mean(floats * floats, axis=-1, keepdims=True) + EPS)
    return (floats * scale * gain.astype(jnp.float32)).astype(jnp.bfloat16)


def expert_weights(rows, group_router, expert_router, named):
    group_logits = jnp.dot(rows, group_router, preferred_element_type=jnp.float32)
    expert_logits = jnp.dot(rows, expert_router, preferred_element_type=jnp.float32)
    groups = group_logits.shape[1]
    experts = expert_logits.shape[1]
    member = (
        jnp.arange(experts, dtype=jnp.int32)[:, None] // (experts // groups)
        == jnp.arange(groups, dtype=jnp.int32)[None, :]
    ).astype(jnp.float32)
    group_exp = jnp.exp(group_logits)
    group_prob = group_exp / jnp.sum(group_exp, axis=1, keepdims=True)
    expert_exp = jnp.exp(expert_logits)
    within = jnp.dot(expert_exp, member, precision=lax.Precision.HIGHEST)
    prob = expert_exp * jnp.dot(group_prob / within, member.T, precision=lax.Precision.HIGHEST)
    picked = [jnp.sum(hot * prob, axis=1, keepdims=True) for hot in named]
    return [value / (picked[0] + picked[1]) for value in picked]


def mixer_half(mixer_input, mixer_gain, pool_in, pool_map, pool_scale, pool_out):
    normed = norm_rows(mixer_input, mixer_gain)
    pooled_in = jnp.dot(normed, pool_in, preferred_element_type=jnp.float32).astype(jnp.bfloat16)
    local_rows = pooled_in.shape[0]
    groups_here = pool_map.shape[0]
    channels = pool_map.shape[1]
    border = passed_along(pooled_in[local_rows - RIM :], "ep", 1)
    padded = jnp.concatenate([border, pooled_in], axis=0).astype(jnp.float32)
    padded = padded.reshape(local_rows + RIM, groups_here, channels)
    leading = lax.axis_index("tp") * groups_here
    windows = jnp.left_shift(jnp.int32(2), leading + jnp.arange(groups_here, dtype=jnp.int32))
    window_sum = jnp.zeros((local_rows, groups_here, channels), jnp.float32)
    for offset in range(RIM + 1):
        active = (offset < windows).astype(jnp.float32)
        window_sum = (
            window_sum + padded[RIM - offset : RIM - offset + local_rows] * active[None, :, None]
        )
    position = lax.axis_index("ep") * local_rows + jnp.arange(local_rows, dtype=jnp.int32)
    counts_here = jnp.minimum(position[:, None] + 1, windows[None, :]).astype(jnp.float32)
    pooled = (window_sum / counts_here[:, :, None] - padded[RIM:]).astype(jnp.bfloat16)
    mapped = jnp.einsum("tgc,gce->tge", pooled, pool_map, preferred_element_type=jnp.float32)
    mixed_rows = (
        mapped.reshape(local_rows, groups_here * channels) * pool_scale.astype(jnp.float32)
    ).astype(jnp.bfloat16)
    return jnp.dot(mixed_rows, pool_out, preferred_element_type=jnp.float32).astype(jnp.bfloat16)


def scattered_sum(partial):
    place = lax.axis_index("tp")
    blocks = lax.axis_size("tp")
    rows, model = partial.shape
    current = partial.reshape(1, blocks, rows // blocks, model)
    for mask in reversed(masks_of("tp")):
        current = current.reshape(-1, 2, rows // blocks, model)
        bit = (place // mask) % 2
        own = lax.dynamic_index_in_dim(current, bit, 1, keepdims=False)
        other = lax.dynamic_index_in_dim(current, 1 - bit, 1, keepdims=False)
        came = swapped(other, "tp", mask)
        current = (own.astype(jnp.float32) + came.astype(jnp.float32)).astype(jnp.bfloat16)
    return current.reshape(rows // blocks, model)


def everyones(shard):
    pieces = [shard]
    for mask in masks_of("tp"):
        pieces = pieces + [swapped(piece, "tp", mask) for piece in pieces]
    return pieces


def on_device(
    mixer_input,
    mixer_gain,
    pool_in,
    pool_map,
    pool_scale,
    pool_out,
    expert_input,
    expert_gain,
    group_router,
    expert_router,
    routes,
    gate_weight,
    up_weight,
    down_weight,
):
    gates = everyones(gate_weight)
    ups = everyones(up_weight)
    downs = everyones(down_weight)

    tp_count = lax.axis_size("tp")
    ep_count = lax.axis_size("ep")
    tp_place = lax.axis_index("tp")
    experts = expert_router.shape[1]
    held = gate_weight.shape[0]
    model = expert_input.shape[1]
    block_len = expert_input.shape[0] // tp_count
    slots = 4 * block_len // experts
    own_input = lax.dynamic_slice_in_dim(expert_input, tp_place * block_len, block_len, 0)
    own_routes = lax.dynamic_slice_in_dim(routes, tp_place * block_len, block_len, 0)
    own_rows = norm_rows(own_input, expert_gain)

    expert_ids = jnp.arange(experts, dtype=jnp.int32)[None, :]
    named = [own_routes[:, j : j + 1] == expert_ids for j in range(2)]
    either = jnp.logical_or(named[0], named[1])
    earlier = jnp.arange(block_len)[:, None] > jnp.arange(block_len)[None, :]
    before = jnp.dot(
        earlier.astype(jnp.bfloat16), either.astype(jnp.bfloat16), preferred_element_type=jnp.float32
    ).astype(jnp.int32)
    place = jnp.where(either, before, -1)
    select = (
        place.T[:, None, :] == jnp.arange(slots, dtype=jnp.int32)[None, :, None]
    ).astype(jnp.bfloat16)
    sending = jnp.dot(
        select.reshape(experts * slots, block_len), own_rows, preferred_element_type=jnp.float32
    ).astype(jnp.bfloat16)
    arrived = lax.all_to_all(sending, "ep", split_axis=0, concat_axis=0, tiled=True)

    mixer_partial = mixer_half(mixer_input, mixer_gain, pool_in, pool_map, pool_scale, pool_out)
    mixer_output = scattered_sum(mixer_partial)

    portions = arrived.reshape(ep_count, held, slots, model)
    results = []
    for own in range(held):
        rows = portions[:, own].reshape(ep_count * slots, model)
        total = None
        for gate_w, up_w, down_w in zip(gates, ups, downs):
            gate = jnp.dot(rows, gate_w[own], preferred_element_type=jnp.float32)
            upward = jnp.dot(rows, up_w[own], preferred_element_type=jnp.float32)
            hidden = (jax.nn.silu(gate) * upward).astype(jnp.bfloat16)
            term = jnp.dot(hidden, down_w[own], preferred_element_type=jnp.float32)
            total = term if total is None else total + term
        results.append(total.astype(jnp.bfloat16).reshape(ep_count, 1, slots, model))
    result = jnp.concatenate(results, axis=1).reshape(ep_count * held * slots, model)
    returned = lax.all_to_all(result, "ep", split_axis=0, concat_axis=0, tiled=True)

    weights = expert_weights(
        own_rows, group_router, expert_router, [hot.astype(jnp.float32) for hot in named]
    )
    slot_ids = jnp.arange(experts * slots, dtype=jnp.int32)[None, :]
    combined = None
    for hot, weight in zip(named, weights):
        target = jnp.sum(jnp.where(hot, expert_ids * slots + before, 0), axis=1, keepdims=True)
        pick = (target == slot_ids).astype(jnp.bfloat16)
        term = jnp.dot(pick, returned, preferred_element_type=jnp.float32) * weight
        combined = term if combined is None else combined + term
    return (mixer_output, combined.astype(jnp.bfloat16))


def solution(mesh):
    return jax.shard_map(
        on_device,
        mesh=mesh,
        in_specs=(
            P("ep", None),
            P(),
            P(None, "tp"),
            P("tp", None, None),
            P("tp"),
            P("tp", None),
            P("ep", None),
            P(),
            P(),
            P(),
            P("ep", None),
            P("ep", None, "tp"),
            P("ep", None, "tp"),
            P("ep", "tp", None),
        ),
        out_specs=(P(("ep", "tp"), None), P(("ep", "tp"), None)),
        check_vma=False,
    )
```

```python
import jax
import jax.numpy as jnp
from jax import lax
from jax.experimental import pallas as pl
from jax.experimental.pallas import tpu as pltpu
from jax.sharding import PartitionSpec as P


RIM = 15
EPS = 1e-06


def passed_along(value, axis, steps):
    count = lax.axis_size(axis)
    leading, last = (max(0, -steps), min(count, count - steps))
    return lax.ppermute(value, axis, [(source, source + steps) for source in range(leading, last)])


def swapped(value, axis, mask):
    count = lax.axis_size(axis)
    return lax.ppermute(value, axis, [(source, source ^ mask) for source in range(count)])


def masks_of(axis):
    count, masks = lax.axis_size(axis), []
    while count > 1:
        count //= 2
        masks.append(count)
    return masks


def norm_rows(values, gain):
    floats = values.astype(jnp.float32)
    scale = lax.rsqrt(jnp.mean(floats * floats, axis=-1, keepdims=True) + EPS)
    return (floats * scale * gain.astype(jnp.float32)).astype(jnp.bfloat16)


def expert_weights(rows, group_router, expert_router, named):
    group_logits = jnp.dot(rows, group_router, preferred_element_type=jnp.float32)
    expert_logits = jnp.dot(rows, expert_router, preferred_element_type=jnp.float32)
    groups = group_logits.shape[1]
    experts = expert_logits.shape[1]
    member = (
        jnp.arange(experts, dtype=jnp.int32)[:, None] // (experts // groups)
        == jnp.arange(groups, dtype=jnp.int32)[None, :]
    ).astype(jnp.float32)
    group_exp = jnp.exp(group_logits)
    group_prob = group_exp / jnp.sum(group_exp, axis=1, keepdims=True)
    expert_exp = jnp.exp(expert_logits)
    within = jnp.dot(expert_exp, member, precision=lax.Precision.HIGHEST)
    prob = expert_exp * jnp.dot(group_prob / within, member.T, precision=lax.Precision.HIGHEST)
    picked = [jnp.sum(hot * prob, axis=1, keepdims=True) for hot in named]
    return [value / (picked[0] + picked[1]) for value in picked]


def mixer_half(mixer_input, mixer_gain, pool_in, pool_map, pool_scale, pool_out):
    normed = norm_rows(mixer_input, mixer_gain)
    pooled_in = jnp.dot(normed, pool_in, preferred_element_type=jnp.float32).astype(jnp.bfloat16)
    local_rows = pooled_in.shape[0]
    groups_here = pool_map.shape[0]
    channels = pool_map.shape[1]
    border = passed_along(pooled_in[local_rows - RIM :], "ep", 1)
    padded = jnp.concatenate([border, pooled_in], axis=0).astype(jnp.float32)
    padded = padded.reshape(local_rows + RIM, groups_here, channels)
    leading = lax.axis_index("tp") * groups_here
    windows = jnp.left_shift(jnp.int32(2), leading + jnp.arange(groups_here, dtype=jnp.int32))
    window_sum = jnp.zeros((local_rows, groups_here, channels), jnp.float32)
    for offset in range(RIM + 1):
        active = (offset < windows).astype(jnp.float32)
        window_sum = (
            window_sum + padded[RIM - offset : RIM - offset + local_rows] * active[None, :, None]
        )
    position = lax.axis_index("ep") * local_rows + jnp.arange(local_rows, dtype=jnp.int32)
    counts_here = jnp.minimum(position[:, None] + 1, windows[None, :]).astype(jnp.float32)
    pooled = (window_sum / counts_here[:, :, None] - padded[RIM:]).astype(jnp.bfloat16)
    mapped = jnp.einsum("tgc,gce->tge", pooled, pool_map, preferred_element_type=jnp.float32)
    mixed_rows = (
        mapped.reshape(local_rows, groups_here * channels) * pool_scale.astype(jnp.float32)
    ).astype(jnp.bfloat16)
    return jnp.dot(mixed_rows, pool_out, preferred_element_type=jnp.float32).astype(jnp.bfloat16)


def scattered_sum(partial):
    place = lax.axis_index("tp")
    blocks = lax.axis_size("tp")
    rows, model = partial.shape
    current = partial.reshape(1, blocks, rows // blocks, model)
    for mask in reversed(masks_of("tp")):
        current = current.reshape(-1, 2, rows // blocks, model)
        bit = (place // mask) % 2
        own = lax.dynamic_index_in_dim(current, bit, 1, keepdims=False)
        other = lax.dynamic_index_in_dim(current, 1 - bit, 1, keepdims=False)
        came = swapped(other, "tp", mask)
        current = (own.astype(jnp.float32) + came.astype(jnp.float32)).astype(jnp.bfloat16)
    return current.reshape(rows // blocks, model)


def spread(shard, masks):
    pieces = [shard]
    for mask in masks:
        pieces = pieces + [swapped(piece, "tp", mask) for piece in pieces]
    return pieces


def hidden_kernel(count, *refs):
    rows_ref, out_ref = refs[0], refs[-1]
    rows = rows_ref[...]
    for index in range(count):
        gate_ref, up_ref = refs[1 + index], refs[1 + count + index]
        width = gate_ref.shape[1]
        gate = jnp.dot(rows, gate_ref[...], preferred_element_type=jnp.float32)
        upward = jnp.dot(rows, up_ref[...], preferred_element_type=jnp.float32)
        hidden = gate / (1.0 + jnp.exp(-gate)) * upward
        out_ref[:, index * width : (index + 1) * width] = hidden.astype(out_ref.dtype)


def hidden_part(rows, gates, ups):
    count = len(gates)
    width = gates[0].shape[1]
    flops = 4 * count * rows.shape[0] * rows.shape[1] * width
    return pl.pallas_call(
        lambda *refs: hidden_kernel(count, *refs),
        out_shape=jax.ShapeDtypeStruct((rows.shape[0], count * width), jnp.bfloat16),
        in_specs=[pl.BlockSpec(memory_space=pltpu.VMEM)] * (1 + 2 * count),
        out_specs=pl.BlockSpec(memory_space=pltpu.VMEM),
        cost_estimate=pl.CostEstimate(
            flops=flops, bytes_accessed=4 * count * rows.shape[1] * width, transcendentals=0
        ),
    )(rows, *gates, *ups)


def result_kernel(halves, *refs):
    out_ref = refs[-1]
    downs = refs[halves:-1]
    total, index = None, 0
    for hidden_ref in refs[:halves]:
        at = 0
        while at < hidden_ref.shape[1]:
            down_ref = downs[index]
            depth = down_ref.shape[0]
            term = jnp.dot(
                hidden_ref[:, at : at + depth], down_ref[...], preferred_element_type=jnp.float32
            )
            total = term if total is None else total + term
            at, index = at + depth, index + 1
    out_ref[...] = total.astype(out_ref.dtype)


def result_part(hiddens, downs):
    rows, columns = hiddens[0].shape[0], downs[0].shape[1]
    depth = sum(down.shape[0] for down in downs)
    return pl.pallas_call(
        lambda *refs: result_kernel(len(hiddens), *refs),
        out_shape=jax.ShapeDtypeStruct((rows, columns), jnp.bfloat16),
        in_specs=[pl.BlockSpec(memory_space=pltpu.VMEM)] * (len(hiddens) + len(downs)),
        out_specs=pl.BlockSpec(memory_space=pltpu.VMEM),
        cost_estimate=pl.CostEstimate(
            flops=2 * rows * depth * columns, bytes_accessed=2 * depth * columns, transcendentals=0
        ),
    )(*hiddens, *downs)


def on_device(
    mixer_input,
    mixer_gain,
    pool_in,
    pool_map,
    pool_scale,
    pool_out,
    expert_input,
    expert_gain,
    group_router,
    expert_router,
    routes,
    gate_weight,
    up_weight,
    down_weight,
):
    masks = masks_of("tp")
    far_mask, near_masks = masks[0], masks[1:]
    parts = 2
    columns = down_weight.shape[2] // parts
    far_gate = swapped(gate_weight, "tp", far_mask)
    far_up = swapped(up_weight, "tp", far_mask)
    own_downs = [down_weight[:, :, part * columns : (part + 1) * columns] for part in range(parts)]
    far_downs = []
    for part in range(parts):
        far_downs.append(swapped(own_downs[part], "tp", far_mask))
    near_gates = spread(gate_weight, near_masks)
    near_ups = spread(up_weight, near_masks)
    near_downs = [spread(down, near_masks) for down in own_downs]

    tp_count = lax.axis_size("tp")
    ep_count = lax.axis_size("ep")
    tp_place = lax.axis_index("tp")
    experts = expert_router.shape[1]
    held = gate_weight.shape[0]
    model = expert_input.shape[1]
    block_len = expert_input.shape[0] // tp_count
    slots = 4 * block_len // experts
    own_input = lax.dynamic_slice_in_dim(expert_input, tp_place * block_len, block_len, 0)
    own_routes = lax.dynamic_slice_in_dim(routes, tp_place * block_len, block_len, 0)
    own_rows = norm_rows(own_input, expert_gain)

    expert_ids = jnp.arange(experts, dtype=jnp.int32)[None, :]
    named = [own_routes[:, j : j + 1] == expert_ids for j in range(2)]
    either = jnp.logical_or(named[0], named[1])
    earlier = jnp.arange(block_len)[:, None] > jnp.arange(block_len)[None, :]
    before = jnp.dot(
        earlier.astype(jnp.bfloat16), either.astype(jnp.bfloat16), preferred_element_type=jnp.float32
    ).astype(jnp.int32)
    place = jnp.where(either, before, -1)
    select = (
        place.T[:, None, :] == jnp.arange(slots, dtype=jnp.int32)[None, :, None]
    ).astype(jnp.bfloat16)
    sending = jnp.dot(
        select.reshape(experts * slots, block_len), own_rows, preferred_element_type=jnp.float32
    ).astype(jnp.bfloat16)
    arrived = lax.all_to_all(sending, "ep", split_axis=0, concat_axis=0, tiled=True)

    mixer_partial = mixer_half(mixer_input, mixer_gain, pool_in, pool_map, pool_scale, pool_out)
    mixer_partial, far_gate, far_up = lax.optimization_barrier((mixer_partial, far_gate, far_up))
    far_gates = spread(far_gate, near_masks)
    far_ups = spread(far_up, near_masks)
    mixer_output = scattered_sum(mixer_partial)

    portions = arrived.reshape(ep_count, held, slots, model)
    rows = [portions[:, own].reshape(ep_count * slots, model) for own in range(held)]
    near_hidden = [
        hidden_part(rows[own], [w[own] for w in near_gates], [w[own] for w in near_ups])
        for own in range(held)
    ]
    near_hidden, far_gates, far_ups = lax.optimization_barrier((near_hidden, far_gates, far_ups))
    far_hidden = [
        hidden_part(rows[own], [w[own] for w in far_gates], [w[own] for w in far_ups])
        for own in range(held)
    ]
    last, returned = far_hidden, []
    for part in range(parts):
        last, far_down = lax.optimization_barrier((last, far_downs[part]))
        if part == 0:
            far_hidden = last
        downs = near_downs[part] + spread(far_down, near_masks)
        last = [
            result_part([near_hidden[own], far_hidden[own]], [w[own] for w in downs])
            for own in range(held)
        ]
        shaped = [value.reshape(ep_count, 1, slots, columns) for value in last]
        joined = shaped[0] if held == 1 else jnp.concatenate(shaped, axis=1)
        returned.append(
            lax.all_to_all(
                joined.reshape(ep_count * held * slots, columns),
                "ep",
                split_axis=0,
                concat_axis=0,
                tiled=True,
            )
        )

    weights = expert_weights(
        own_rows, group_router, expert_router, [hot.astype(jnp.float32) for hot in named]
    )
    slot_ids = jnp.arange(experts * slots, dtype=jnp.int32)[None, :]
    picks = []
    for hot in named:
        target = jnp.sum(jnp.where(hot, expert_ids * slots + before, 0), axis=1, keepdims=True)
        picks.append((target == slot_ids).astype(jnp.bfloat16))
    outputs = []
    for value in returned:
        combined = None
        for pick, weight in zip(picks, weights):
            term = jnp.dot(pick, value, preferred_element_type=jnp.float32) * weight
            combined = term if combined is None else combined + term
        outputs.append(combined.astype(jnp.bfloat16))
    return (mixer_output, jnp.concatenate(outputs, axis=1))


def solution(mesh):
    return jax.shard_map(
        on_device,
        mesh=mesh,
        in_specs=(
            P("ep", None),
            P(),
            P(None, "tp"),
            P("tp", None, None),
            P("tp"),
            P("tp", None),
            P("ep", None),
            P(),
            P(),
            P(),
            P("ep", None),
            P("ep", None, "tp"),
            P("ep", None, "tp"),
            P("ep", "tp", None),
        ),
        out_specs=(P(("ep", "tp"), None), P(("ep", "tp"), None)),
        check_vma=False,
    )
```

```python
import jax
import jax.numpy as jnp
from jax import lax
from jax.experimental import pallas as pl
from jax.experimental.pallas import tpu as pltpu
from jax.sharding import PartitionSpec as P


RIM = 15
EPS = 1e-06


def passed_along(value, axis, steps):
    count = lax.axis_size(axis)
    leading, last = (max(0, -steps), min(count, count - steps))
    return lax.ppermute(value, axis, [(source, source + steps) for source in range(leading, last)])


def swapped(value, axis, mask):
    count = lax.axis_size(axis)
    return lax.ppermute(value, axis, [(source, source ^ mask) for source in range(count)])


def masks_of(axis):
    count, masks = lax.axis_size(axis), []
    while count > 1:
        count //= 2
        masks.append(count)
    return masks


def norm_rows(values, gain):
    floats = values.astype(jnp.float32)
    scale = lax.rsqrt(jnp.mean(floats * floats, axis=-1, keepdims=True) + EPS)
    return (floats * scale * gain.astype(jnp.float32)).astype(jnp.bfloat16)


def expert_weights(rows, group_router, expert_router, named):
    group_logits = jnp.dot(rows, group_router, preferred_element_type=jnp.float32)
    expert_logits = jnp.dot(rows, expert_router, preferred_element_type=jnp.float32)
    groups = group_logits.shape[1]
    experts = expert_logits.shape[1]
    member = (
        jnp.arange(experts, dtype=jnp.int32)[:, None] // (experts // groups)
        == jnp.arange(groups, dtype=jnp.int32)[None, :]
    ).astype(jnp.float32)
    group_exp = jnp.exp(group_logits)
    group_prob = group_exp / jnp.sum(group_exp, axis=1, keepdims=True)
    expert_exp = jnp.exp(expert_logits)
    within = jnp.dot(expert_exp, member, precision=lax.Precision.HIGHEST)
    prob = expert_exp * jnp.dot(group_prob / within, member.T, precision=lax.Precision.HIGHEST)
    picked = [jnp.sum(hot * prob, axis=1, keepdims=True) for hot in named]
    return [value / (picked[0] + picked[1]) for value in picked]


def mixer_half(pooled_in, border, pool_map, pool_scale, pool_out):
    local_rows = pooled_in.shape[0]
    groups_here = pool_map.shape[0]
    channels = pool_map.shape[1]
    padded = jnp.concatenate([border, pooled_in], axis=0).astype(jnp.float32)
    padded = padded.reshape(local_rows + RIM, groups_here, channels)
    leading = lax.axis_index("tp") * groups_here
    windows = jnp.left_shift(jnp.int32(2), leading + jnp.arange(groups_here, dtype=jnp.int32))
    window_sum = jnp.zeros((local_rows, groups_here, channels), jnp.float32)
    for offset in range(RIM + 1):
        active = (offset < windows).astype(jnp.float32)
        window_sum = (
            window_sum + padded[RIM - offset : RIM - offset + local_rows] * active[None, :, None]
        )
    position = lax.axis_index("ep") * local_rows + jnp.arange(local_rows, dtype=jnp.int32)
    counts_here = jnp.minimum(position[:, None] + 1, windows[None, :]).astype(jnp.float32)
    pooled = (window_sum / counts_here[:, :, None] - padded[RIM:]).astype(jnp.bfloat16)
    mapped = jnp.einsum("tgc,gce->tge", pooled, pool_map, preferred_element_type=jnp.float32)
    mixed_rows = (
        mapped.reshape(local_rows, groups_here * channels) * pool_scale.astype(jnp.float32)
    ).astype(jnp.bfloat16)
    return jnp.dot(mixed_rows, pool_out, preferred_element_type=jnp.float32).astype(jnp.bfloat16)


def scattered_sum(partial):
    place = lax.axis_index("tp")
    blocks = lax.axis_size("tp")
    rows, model = partial.shape
    current = partial.reshape(1, blocks, rows // blocks, model)
    for mask in reversed(masks_of("tp")):
        current = current.reshape(-1, 2, rows // blocks, model)
        bit = (place // mask) % 2
        own = lax.dynamic_index_in_dim(current, bit, 1, keepdims=False)
        other = lax.dynamic_index_in_dim(current, 1 - bit, 1, keepdims=False)
        came = swapped(other, "tp", mask)
        current = (own.astype(jnp.float32) + came.astype(jnp.float32)).astype(jnp.bfloat16)
    return current.reshape(rows // blocks, model)


def spread(shard, masks):
    pieces = [shard]
    for mask in masks:
        pieces = pieces + [swapped(piece, "tp", mask) for piece in pieces]
    return pieces


def hidden_kernel(pieces, count, *refs):
    sources, out_ref = refs[: pieces + 2 * count], refs[pieces + 2 * count]
    rows_buf, weight_buf, sem = refs[pieces + 2 * count + 1 :]
    length = rows_buf.shape[0] // pieces
    targets = [rows_buf.at[pl.ds(index * length, length)] for index in range(pieces)]
    targets += [weight_buf.at[index] for index in range(2 * count)]
    copies = [
        pltpu.make_async_copy(source, target, sem.at[index])
        for index, (source, target) in enumerate(zip(sources, targets))
    ]
    for copy in copies:
        copy.start()
    for copy in copies[:pieces]:
        copy.wait()
    rows = rows_buf[...]
    width = weight_buf.shape[2]
    for index in range(count):
        copies[pieces + 2 * index].wait()
        gate = jnp.dot(rows, weight_buf[2 * index], preferred_element_type=jnp.float32)
        copies[pieces + 2 * index + 1].wait()
        upward = jnp.dot(rows, weight_buf[2 * index + 1], preferred_element_type=jnp.float32)
        hidden = gate / (1.0 + jnp.exp(-gate)) * upward
        out_ref[:, index * width : (index + 1) * width] = hidden.astype(out_ref.dtype)


def hidden_part(pieces, gates, ups):
    count, parts = len(gates), len(pieces)
    depth, width = gates[0].shape
    rows = parts * pieces[0].shape[0]
    weights = [array for pair in zip(gates, ups) for array in pair]
    return pl.pallas_call(
        lambda *refs: hidden_kernel(parts, count, *refs),
        out_shape=jax.ShapeDtypeStruct((rows, count * width), jnp.bfloat16),
        in_specs=[pl.BlockSpec(memory_space=pl.ANY)] * (parts + 2 * count),
        out_specs=pl.BlockSpec(memory_space=pltpu.VMEM),
        scratch_shapes=[
            pltpu.VMEM((rows, depth), jnp.bfloat16),
            pltpu.VMEM((2 * count, depth, width), jnp.bfloat16),
            pltpu.SemaphoreType.DMA((parts + 2 * count,)),
        ],
        cost_estimate=pl.CostEstimate(
            flops=4 * count * rows * depth * width,
            bytes_accessed=4 * count * depth * width,
            transcendentals=0,
        ),
    )(*pieces, *weights)


def result_kernel(halves, count, parts, *refs):
    hiddens, downs = refs[:halves], refs[halves : halves + count]
    outs = refs[halves + count : halves + count + parts]
    down_buf, sem = refs[halves + count + parts :]
    copies = [
        pltpu.make_async_copy(source, down_buf.at[index], sem.at[index])
        for index, source in enumerate(downs)
    ]
    for copy in copies:
        copy.start()
    depth = down_buf.shape[1]
    total, index = None, 0
    for hidden_ref in hiddens:
        for at in range(0, hidden_ref.shape[1], depth):
            copies[index].wait()
            term = jnp.dot(
                hidden_ref[:, at : at + depth], down_buf[index], preferred_element_type=jnp.float32
            )
            total = term if total is None else total + term
            index += 1
    length = outs[0].shape[0]
    for index, out_ref in enumerate(outs):
        out_ref[...] = total[index * length : (index + 1) * length].astype(out_ref.dtype)


def result_part(hiddens, downs, parts):
    rows, (depth, columns) = hiddens[0].shape[0], downs[0].shape
    return pl.pallas_call(
        lambda *refs: result_kernel(len(hiddens), len(downs), parts, *refs),
        out_shape=[jax.ShapeDtypeStruct((rows // parts, columns), jnp.bfloat16)] * parts,
        in_specs=[pl.BlockSpec(memory_space=pltpu.VMEM)] * len(hiddens)
        + [pl.BlockSpec(memory_space=pl.ANY)] * len(downs),
        out_specs=[pl.BlockSpec(memory_space=pltpu.VMEM)] * parts,
        scratch_shapes=[
            pltpu.VMEM((len(downs), depth, columns), jnp.bfloat16),
            pltpu.SemaphoreType.DMA((len(downs),)),
        ],
        cost_estimate=pl.CostEstimate(
            flops=2 * rows * depth * len(downs) * columns,
            bytes_accessed=2 * depth * len(downs) * columns,
            transcendentals=0,
        ),
    )(*hiddens, *downs)


def pooled_rows(mixer_input, mixer_gain, pool_in):
    normed = norm_rows(mixer_input, mixer_gain)
    pooled_in = jnp.dot(normed, pool_in, preferred_element_type=jnp.float32).astype(jnp.bfloat16)
    border = passed_along(pooled_in[pooled_in.shape[0] - RIM :], "ep", 1)
    return pooled_in, border


def on_device(
    mixer_input,
    mixer_gain,
    pool_in,
    pool_map,
    pool_scale,
    pool_out,
    expert_input,
    expert_gain,
    group_router,
    expert_router,
    routes,
    gate_weight,
    up_weight,
    down_weight,
):
    masks = masks_of("tp")
    far_mask, near_masks = masks[0], masks[1:]
    parts = 2
    columns = down_weight.shape[2] // parts
    far_gate = swapped(gate_weight, "tp", far_mask)
    far_up = swapped(up_weight, "tp", far_mask)
    own_downs = [down_weight[:, :, part * columns : (part + 1) * columns] for part in range(parts)]
    far_downs = []
    for part in range(parts):
        far_downs.append(swapped(own_downs[part], "tp", far_mask))
    near_gates = spread(gate_weight, near_masks)
    near_ups = spread(up_weight, near_masks)
    near_downs = [spread(down, near_masks) for down in own_downs]

    tp_count = lax.axis_size("tp")
    ep_count = lax.axis_size("ep")
    tp_place = lax.axis_index("tp")
    experts = expert_router.shape[1]
    held = gate_weight.shape[0]
    model = expert_input.shape[1]
    block_len = expert_input.shape[0] // tp_count
    slots = 4 * block_len // experts
    own_input = lax.dynamic_slice_in_dim(expert_input, tp_place * block_len, block_len, 0)
    own_routes = lax.dynamic_slice_in_dim(routes, tp_place * block_len, block_len, 0)
    own_rows = norm_rows(own_input, expert_gain)

    expert_ids = jnp.arange(experts, dtype=jnp.int32)[None, :]
    named = [own_routes[:, j : j + 1] == expert_ids for j in range(2)]
    either = jnp.logical_or(named[0], named[1])
    earlier = jnp.arange(block_len)[:, None] > jnp.arange(block_len)[None, :]
    before = jnp.dot(
        earlier.astype(jnp.bfloat16), either.astype(jnp.bfloat16), preferred_element_type=jnp.float32
    ).astype(jnp.int32)
    place = jnp.where(either, before, -1)
    ep_place = lax.axis_index("ep")
    direct = ep_count <= 8 and held == 1 and ep_count & (ep_count - 1) == 0
    order = expert_ids[0] ^ ep_place if direct else expert_ids[0]
    block_of = expert_ids ^ ep_place if direct else expert_ids
    wanted = jnp.sum(
        jnp.where(order[:, None, None] == expert_ids[:, :, None], place.T[None, :, :], 0), axis=1
    )
    select = (
        wanted[:, None, :] == jnp.arange(slots, dtype=jnp.int32)[None, :, None]
    ).astype(jnp.bfloat16)
    sending = jnp.dot(
        select.reshape(experts * slots, block_len), own_rows, preferred_element_type=jnp.float32
    ).astype(jnp.bfloat16)
    ranks = sorted(range(1, ep_count), key=lambda k: (-bin(k).count("1"), -k))

    def exchanged(pieces):
        came = [pieces[0]] + [None] * (ep_count - 1)
        for k in ranks:
            came[k] = swapped(pieces[k], "ep", k)
        return came

    if direct:
        arrived = exchanged([sending[k * slots : (k + 1) * slots] for k in range(ep_count)])
        rows = [arrived]
    else:
        arrived = lax.all_to_all(sending, "ep", split_axis=0, concat_axis=0, tiled=True)
        portions = arrived.reshape(ep_count, held, slots, model)
        rows = [[portions[:, own].reshape(ep_count * slots, model)] for own in range(held)]

    pooled_in, border = pooled_rows(mixer_input, mixer_gain, pool_in)
    far_gates = spread(far_gate, near_masks)
    far_ups = spread(far_up, near_masks)
    near_hidden = [
        hidden_part(rows[own], [w[own] for w in near_gates], [w[own] for w in near_ups])
        for own in range(held)
    ]
    near_hidden, far_gates, far_ups = lax.optimization_barrier((near_hidden, far_gates, far_ups))
    far_hidden = [
        hidden_part(rows[own], [w[own] for w in far_gates], [w[own] for w in far_ups])
        for own in range(held)
    ]
    last, returned = far_hidden, []
    for part in range(parts):
        if part == 0:
            far_hidden, far_down = lax.optimization_barrier((last, far_downs[part]))
        else:
            far_down, mixer_partial = lax.optimization_barrier((far_downs[part], mixer_partial))
            mixer_output = scattered_sum(mixer_partial)
        downs = near_downs[part] + spread(far_down, near_masks)
        last = [
            result_part(
                [near_hidden[own], far_hidden[own]], [w[own] for w in downs], len(rows[own])
            )
            for own in range(held)
        ]
        if part == 0:
            last, border = lax.optimization_barrier((last, border))
            mixer_partial = mixer_half(pooled_in, border, pool_map, pool_scale, pool_out)
        if part and direct:
            returned[-1], _ = lax.optimization_barrier((returned[-1], last))
        if direct:
            returned.append(exchanged(last[0]))
        else:
            shaped = [value[0].reshape(ep_count, 1, slots, columns) for value in last]
            joined = shaped[0] if held == 1 else jnp.concatenate(shaped, axis=1)
            joined = joined.reshape(ep_count * held * slots, columns)
            returned.append([lax.all_to_all(joined, "ep", split_axis=0, concat_axis=0, tiled=True)])

    weights = expert_weights(
        own_rows, group_router, expert_router, [hot.astype(jnp.float32) for hot in named]
    )
    slot_ids = jnp.arange(experts * slots, dtype=jnp.int32)[None, :]
    picks = []
    for hot in named:
        target = jnp.sum(jnp.where(hot, block_of * slots + before, 0), axis=1, keepdims=True)
        picks.append((target == slot_ids).astype(jnp.bfloat16))
    outputs = []
    for came in returned:
        value = jnp.concatenate(came, axis=0)
        combined = None
        for pick, weight in zip(picks, weights):
            term = jnp.dot(pick, value, preferred_element_type=jnp.float32) * weight
            combined = term if combined is None else combined + term
        outputs.append(combined.astype(jnp.bfloat16))
    return (mixer_output, jnp.concatenate(outputs, axis=1))


def solution(mesh):
    return jax.shard_map(
        on_device,
        mesh=mesh,
        in_specs=(
            P("ep", None),
            P(),
            P(None, "tp"),
            P("tp", None, None),
            P("tp"),
            P("tp", None),
            P("ep", None),
            P(),
            P(),
            P(),
            P("ep", None),
            P("ep", None, "tp"),
            P("ep", None, "tp"),
            P("ep", "tp", None),
        ),
        out_specs=(P(("ep", "tp"), None), P(("ep", "tp"), None)),
        check_vma=False,
    )
```
